32 devices in a mesh: ep: 8 (over z, y), tp: 4 (over x, core).
Axes of the slice: x: 2, y: 2, z: 4, core: 2. Of those that a mesh axis runs over, the one named last changes fastest.
Arguments:
- queries: bfloat16 [2048, 2048], P('ep', 'tp'), may hold values from -150 to 150, as said below
- keys: bfloat16 [2048, 512], P('ep', 'tp'), may hold values from -6 to 6
- values: bfloat16 [2048, 512], P('ep', 'tp'), may hold values from -6 to 6
- cum_gates: float32 [2048, 16], P('ep', 'tp'), may hold values from -2048 to 0, as said below
- out_proj: bfloat16 [2048, 4096], P('tp'), may hold values from -0.125 to 0.125
- tokens: bfloat16 [1024, 4096], P('ep'), may hold values from -6 to 6
- norm_gain: float32 [4096], replicated, may hold values from 0.1 to 1.9
- routes: int32 [1024, 4], P('ep'), may hold values from 0 to 7, all different within a row; in each aligned block of 128 rows (0 to 127, 128 to 255, ...) at most 128 rows name the same one
- route_weights: float32 [1024, 4], P('ep'), may hold values from 0.2 to 1
- w_gate: bfloat16 [8, 4096, 1024], P('ep', None, 'tp'), may hold values from -0.09375 to 0.09375
- w_up: bfloat16 [8, 4096, 1024], P('ep', None, 'tp'), may hold values from -0.09375 to 0.09375
- w_down: bfloat16 [8, 1024, 4096], P('ep', 'tp'), may hold values from -0.1875 to 0.1875
Outputs:
- attn_mixed: bfloat16 [2048, 4096], P(('ep', 'tp'))
- moe_out: bfloat16 [1024, 4096], P('ep', 'tp')
The draws below stay inside these ranges and needn't reach their ends.
Inputs may be any that keep to these rules, and one draw needn't show every extreme that they name: keys and queries are of order one except where the draw sets a few queries far larger. `cum_gates`: never rises along positions. `routes`: each row names 4 different experts; among the rows of one index of ep no expert is named by more than 128 rows, a bound that some block reaches in some of them.
All inputs are finite; a program needn't handle non-finite values.
Results may differ from the reference program's by a relative error of at most 0.0109.
Values may be sent and summed in bfloat16 or wider, within the bound.
A program may use at most 128 MiB of HBM per device.

```python
import math
import jax
import jax.numpy as jnp
import numpy as np
from jax import lax

D = 4096
QH = 16
KVH = 4
HD = 128
DE = 1024
TOPK = 4
A_TOK = 256
E_TOK = 128
CONTEXT_SPAN = 2048
EXPERTS = 8
CAP = 128
N_EP = 8
N_TP = 4


def drawn_pair(key):
    query_base = jnp.clip(jax.random.normal(jax.random.fold_in(key, 11), (CONTEXT_SPAN, QH * HD), jnp.float32), -5.0, 5.0)
    key_base = jnp.clip(jax.random.normal(jax.random.fold_in(key, 12), (CONTEXT_SPAN, KVH * HD), jnp.float32), -5.0, 5.0)
    return (query_base, key_base)


def draw_queries(key, part):
    return drawn_pair(key)[0].astype(jnp.bfloat16)


def draw_keys(key, part):
    return drawn_pair(key)[1].astype(jnp.bfloat16)


def draw_cum_gates(key, part):
    order = jax.random.permutation(jax.random.fold_in(key, 21), QH)
    fast_count = QH // 2
    rapid_fading = (order < fast_count).astype(jnp.float32)
    fast_rate = jnp.exp(jax.random.uniform(jax.random.fold_in(key, 22), (QH,), jnp.float32, math.log(1.0 / 60.0), math.log(1.0 / 20.0)))
    slow_rate = jnp.exp(jax.random.uniform(jax.random.fold_in(key, 23), (QH,), jnp.float32, math.log(0.2), math.log(0.8))) / CONTEXT_SPAN
    rate = rapid_fading * fast_rate + (1.0 - rapid_fading) * slow_rate
    block_factor = jnp.exp(jax.random.uniform(jax.random.fold_in(key, 24), (CONTEXT_SPAN // A_TOK,), jnp.float32, math.log(0.5), math.log(2.0)))
    factor = jnp.repeat(block_factor, A_TOK)
    rough = jax.random.uniform(jax.random.fold_in(key, 25), (CONTEXT_SPAN, QH), jnp.float32, 0.2, 1.8)
    retention_logit = -rate[None, :] * factor[:, None] * rough
    flagged_indices = jax.random.randint(jax.random.fold_in(key, 26), (3,), 0, CONTEXT_SPAN)
    spike_occasions = jnp.zeros((CONTEXT_SPAN,), jnp.float32).at[flagged_indices].add(1.0)
    discarded_items = jnp.log(jax.random.uniform(jax.random.fold_in(key, 27), (QH,), jnp.float32, 0.55, 0.8))
    retention_logit = retention_logit + spike_occasions[:, None] * discarded_items[None, :] * (1.0 - rapid_fading)[None, :]
    return jnp.cumsum(retention_logit, axis=0)


def shard_levels(rng, extent, cuts, least, top_value):
    def one(dim, shards_of):
        steps = jax.random.uniform(jax.random.fold_in(jax.random.fold_in(rng, 6), dim), (shards_of,), jnp.float32, least / len(cuts), top_value / len(cuts))
        return jnp.repeat(jnp.exp(steps), extent[dim] // shards_of).reshape((-1,) + (1,) * (len(extent) - dim - 1))

    level = one(*cuts[0])
    for cut in cuts[1:]:
        level = level * one(*cut)
    return level


def assign_block(own_key, own, number, rows, number_of, top, bound, slope):
    sequence = jax.random.permutation(own_key, number_of)
    crowded, ordinary = load_shares(number_of, rows * top, bound, slope, True), load_shares(number_of, rows * top, bound, slope, False)
    places = jnp.arange(number_of)

    def named(tallies, rotation):
        used = int((tallies > 0).sum())
        fixed = max(1, used // 4)
        shifted = fixed + (places - fixed + rotation * (used - fixed)) % max(1, number_of - fixed)
        return jnp.zeros((number_of,), jnp.int32).at[sequence[jnp.where(places < fixed, places, shifted)]].set(jnp.asarray(tallies, jnp.int32))

    tallies = jnp.where(number % 4 == 0, named(crowded, number // 4), named(ordinary, number - number // 4 - 1))
    mixed = jax.random.permutation(jax.random.fold_in(own, 3), number_of)
    donor, taker = mixed[0:number_of // 2 * 2:2], mixed[1:number_of // 2 * 2:2]
    slack = jnp.minimum(tallies[donor] - 1, bound - tallies[taker]) // 2
    slack = jnp.where((donor == sequence[0]) | (taker == sequence[0]) | (tallies[taker] == 0), 0, jnp.maximum(slack, 0))
    shifted = jax.random.randint(jax.random.fold_in(own, 4), (number_of // 2,), 0, 1 << 20) % (slack + 1)
    tallies = tallies.at[donor].add(-shifted).at[taker].add(shifted)
    labels = jnp.searchsorted(jnp.cumsum(tallies), jnp.arange(rows * top), side="right").astype(jnp.int32)
    table = labels.reshape(top, rows).T
    table = table[jax.random.permutation(jax.random.fold_in(own, 1), rows)]
    rotation = jax.random.randint(jax.random.fold_in(own, 2), (rows, 1), 0, top)
    return jnp.take_along_axis(table, (jnp.arange(top)[None, :] + rotation) % top, axis=1)


def load_shares(amount, total, most, skew, full):
    loads = [(1 << 20) // math.isqrt(grade ** skew) + 1 for grade in range(1, amount + 1)]
    largest = most if full else min(most, max(-(-total // amount), total * loads[0] // sum(loads)))
    least = 1 if total - largest >= amount - 1 else 0
    holding, surplus = [largest] + [least] * (amount - 1), total - largest - least * (amount - 1)
    while surplus > 0:
        movable = [i for i in range(1, amount) if holding[i] < largest] or [i for i in range(1, amount) if holding[i] < most]
        whole, left = sum([loads[i] for i in movable]), surplus
        for i in movable:
            extra = min(most - holding[i], max(1, left * loads[i] // whole), surplus)
            holding[i] = holding[i] + extra
            surplus = surplus - extra
    return np.array(holding)


def scatter_about(own_key, dims, deviation, limit, pieces=(), kind=jnp.bfloat16):
    drawn = deviation * jax.random.normal(own_key, dims, jnp.float32)
    if pieces:
        drawn = drawn * shard_levels(own_key, dims, pieces, -0.22, 0.18)
    return jnp.clip(drawn, -limit, limit).astype(kind)


def setup_inputs(seed: int = 0) -> dict:
    arg_keys = jax.random.split(jax.random.key(seed), 13)
    queries = draw_queries(jax.random.fold_in(arg_keys[12], 71), 0)
    keys = draw_keys(jax.random.fold_in(arg_keys[12], 71), 0)
    values = scatter_about(arg_keys[2], (CONTEXT_SPAN, KVH * HD), 1.0, 6.0, ((0, 8), (1, 4)))
    cum_gates = draw_cum_gates(jax.random.fold_in(arg_keys[12], 71), 0)
    out_proj = scatter_about(arg_keys[4], (QH * HD, D), (QH * HD) ** -0.5, 0.125, ((0, 4),))
    tokens = scatter_about(arg_keys[5], (E_TOK * N_EP, D), 1.0, 6.0, ((0, 8),))
    norm_gain = jnp.clip(1.0 + 0.18 * jax.random.normal(arg_keys[6], (D,), jnp.float32), 0.1, 1.9)
    routes_keys = jax.random.split(jax.random.fold_in(arg_keys[7], 1), (E_TOK * N_EP) // E_TOK)
    routes_turns = jax.random.permutation(jax.random.fold_in(arg_keys[7], 3), (E_TOK * N_EP) // E_TOK)
    routes = jax.vmap(lambda own, number: assign_block(jax.random.fold_in(arg_keys[7], 2), own, number, E_TOK, EXPERTS, TOPK, CAP, 1))(routes_keys, routes_turns).reshape((E_TOK * N_EP, TOPK))
    route_weights = jnp.clip(0.2 + 0.8 * jax.random.uniform(arg_keys[8], (E_TOK * N_EP, TOPK), jnp.float32) ** shard_levels(arg_keys[8], (E_TOK * N_EP, TOPK), ((0, 8),), -0.2, 0.2), 0.2, 1.0)
    w_gate = scatter_about(arg_keys[9], (EXPERTS, D, DE), D ** -0.5, 0.09375, ((0, 8), (2, 4)))
    w_up = scatter_about(arg_keys[10], (EXPERTS, D, DE), D ** -0.5, 0.09375, ((0, 8), (2, 4)))
    w_down = scatter_about(arg_keys[11], (EXPERTS, DE, D), DE ** -0.5, 0.1875, ((0, 8), (1, 4)))
    return {"queries": queries, "keys": keys, "values": values, "cum_gates": cum_gates, "out_proj": out_proj, "tokens": tokens, "norm_gain": norm_gain, "routes": routes, "route_weights": route_weights, "w_gate": w_gate, "w_up": w_up, "w_down": w_down}


def attention_part(queries, keys, values, cum_gates, out_proj):
    group_ratio = QH // KVH
    score_scale = HD ** (-0.5)
    query_wide = queries.astype(jnp.float32).reshape(CONTEXT_SPAN, QH, HD)
    key_wide = jnp.repeat(keys.astype(jnp.float32).reshape(CONTEXT_SPAN, KVH, HD), group_ratio, axis=1)
    value_wide = jnp.repeat(values.astype(jnp.float32).reshape(CONTEXT_SPAN, KVH, HD), group_ratio, axis=1)
    gate_heads = cum_gates.T
    block_len = math.gcd(CONTEXT_SPAN, 512)
    outputs = []
    for block_index in range(CONTEXT_SPAN // block_len):
        row_begin = block_index * block_len
        row_end = row_begin + block_len
        scores = jnp.einsum('qhd,khd->hqk', query_wide[row_begin:row_end], key_wide[:row_end]) * score_scale
        scores = scores + gate_heads[:, row_begin:row_end, None] - gate_heads[:, None, :row_end]
        query_pos = row_begin + jnp.arange(block_len, dtype=jnp.int32)
        key_pos = jnp.arange(row_end, dtype=jnp.int32)
        allowed = key_pos[None, :] <= query_pos[:, None]
        scores = jnp.where(allowed[None], scores, -jnp.inf)
        largest = lax.optimization_barrier(jnp.max(scores, axis=-1, keepdims=True))
        weights = jnp.exp(scores - largest)
        totals = lax.optimization_barrier(jnp.sum(weights, axis=-1))
        rounded = lax.optimization_barrier(weights.astype(jnp.bfloat16)).astype(jnp.float32)
        weighted = jnp.einsum('hqk,khd->qhd', rounded, value_wide[:row_end])
        outputs.append((weighted / totals.T[:, :, None]).astype(jnp.bfloat16))
    heads_out = jnp.concatenate(outputs, axis=0).reshape(CONTEXT_SPAN, QH * HD)
    group_width = QH * HD // N_TP
    summed = jnp.zeros((CONTEXT_SPAN, D), jnp.float32)
    for part_index in range(N_TP):
        column_first = part_index * group_width
        col_end = column_first + group_width
        partial_value = jnp.dot(heads_out[:, column_first:col_end], out_proj[column_first:col_end], preferred_element_type=jnp.float32)
        summed = summed + lax.optimization_barrier(partial_value.astype(jnp.bfloat16)).astype(jnp.float32)
    return summed.astype(jnp.bfloat16)

def expert_portion(tokens, norm_gain, routes, route_weights, w_gate, w_up, w_down):
    tokens_wide = tokens.astype(jnp.float32)
    normed = (tokens_wide * lax.rsqrt(lax.optimization_barrier(jnp.mean(tokens_wide * tokens_wide, axis=-1, keepdims=True)) + 1e-06) * norm_gain.astype(jnp.float32)).astype(jnp.bfloat16)
    id_grid = routes.reshape(N_EP, E_TOK * TOPK)
    onehot = (id_grid[..., None] == jnp.arange(EXPERTS, dtype=jnp.int32)).astype(jnp.int32)
    slot_rank = lax.optimization_barrier(jnp.sum((jnp.cumsum(onehot, axis=1) - 1) * onehot, axis=2))
    source = jnp.arange(N_EP, dtype=jnp.int32)[:, None]
    position = source * CAP + slot_rank
    owner_row = source * E_TOK + jnp.arange(E_TOK * TOPK, dtype=jnp.int32)[None, :] // TOPK
    slot_rows = jnp.full((EXPERTS, N_EP * CAP), -1, jnp.int32)
    slot_rows = slot_rows.at[id_grid.reshape(-1), position.reshape(-1)].set(owner_row.reshape(-1))
    quarter = DE // N_TP

    def one_expert(packed):
        row_ids, gate_weight, up_weight, down_weight = packed
        filled = row_ids >= 0
        gathered = jnp.where(filled[:, None], normed[jnp.maximum(row_ids, 0)], jnp.zeros((), jnp.bfloat16))
        gate_act = jnp.dot(gathered, gate_weight, preferred_element_type=jnp.float32)
        up_act = jnp.dot(gathered, up_weight, preferred_element_type=jnp.float32)
        latent_width = (jax.nn.silu(gate_act) * up_act).astype(jnp.bfloat16)
        summed = jnp.zeros((row_ids.shape[0], D), jnp.float32)
        for part_index in range(N_TP):
            column_first = part_index * quarter
            partial_value = jnp.dot(latent_width[:, column_first:column_first + quarter], down_weight[column_first:column_first + quarter], preferred_element_type=jnp.float32)
            summed = summed + lax.optimization_barrier(partial_value.astype(jnp.bfloat16)).astype(jnp.float32)
        return summed.astype(jnp.bfloat16)
    results = lax.map(one_expert, (slot_rows, w_gate, w_up, w_down))
    picked = results[id_grid.reshape(-1), position.reshape(-1)].astype(jnp.float32).reshape(N_EP * E_TOK, TOPK, D)
    return lax.optimization_barrier(jnp.sum(picked * route_weights[:, :, None], axis=1)).astype(jnp.bfloat16)

def reference(queries, keys, values, cum_gates, out_proj, tokens, norm_gain, routes, route_weights, w_gate, w_up, w_down):
    attn_mixed = attention_part(queries, keys, values, cum_gates, out_proj)
    moe_out = expert_portion(tokens, norm_gain, routes, route_weights, w_gate, w_up, w_down)
    return (attn_mixed, moe_out)
```

```python
import math

import jax
import jax.numpy as jnp
from jax import lax
from jax.sharding import PartitionSpec as P

HD = 128


SCORE_FLOOR = -1e30


def split_three(x):
    high = lax.reduce_precision(x, 8, 7)
    rest = x - high
    middle = lax.reduce_precision(rest, 8, 7)
    low = rest - middle
    return jnp.stack([high, middle, low]).astype(jnp.bfloat16)


def join_three(pieces, axis):
    wide = pieces.astype(jnp.float32)
    parts = [lax.index_in_dim(wide, i, axis, keepdims=False) for i in range(3)]
    return (parts[2] + parts[1]) + parts[0]


def gather_packed(arrays, axis):
    lanes = 128
    rows = []
    for array in arrays:
        flat = array.reshape(-1)
        flat = jnp.pad(flat, (0, -flat.shape[0] % (16 * lanes)))
        rows.append(flat.reshape(-1, lanes))
    gathered = lax.all_gather(jnp.concatenate(rows, axis=0), axis, axis=0, tiled=False)
    count = gathered.shape[0]
    results = []
    first = 0
    for array, block in zip(arrays, rows):
        piece = gathered[:, first : first + block.shape[0]]
        if array.size != block.size:
            piece = piece.reshape(count, -1)[:, : array.size]
        results.append(piece.reshape((count,) + array.shape))
        first += block.shape[0]
    return results


def attend(queries, key_rows, value_rows, key_gates, cum_gates, out_proj):
    local_rows = queries.shape[0]
    groups = key_rows.shape[1] // HD
    group_ratio = cum_gates.shape[1] // groups
    score_scale = HD ** (-0.5)
    first_row = lax.axis_index("ep") * local_rows
    last_row = first_row + local_rows - 1
    query_four = queries.reshape(local_rows, groups, group_ratio, HD)
    query_gate = cum_gates.reshape(local_rows, groups, group_ratio)
    query_pos = first_row + jnp.arange(local_rows, dtype=jnp.int32)
    initial = (
        jnp.full((local_rows, groups, group_ratio), SCORE_FLOOR, jnp.float32),
        jnp.zeros((local_rows, groups, group_ratio), jnp.float32),
        jnp.zeros((local_rows, groups, group_ratio, HD), jnp.float32),
    )
    length = key_rows.shape[0]
    block_len = math.gcd(length, 512)

    def advance(block_index, state):
        offset = block_index * block_len

        def accumulate(current):
            maxima, totals, weighted = current
            key_block = lax.dynamic_slice_in_dim(key_rows, offset, block_len, 0).reshape(
                block_len, groups, HD
            )
            value_block = lax.dynamic_slice_in_dim(value_rows, offset, block_len, 0).reshape(
                block_len, groups, HD
            )
            gate_block = lax.dynamic_slice_in_dim(key_gates, offset, block_len, 0).reshape(
                block_len, groups, group_ratio
            )
            scores = (
                jnp.einsum(
                    "qgrd,kgd->qgrk", query_four, key_block, preferred_element_type=jnp.float32
                )
                * score_scale
            )
            scores = scores + query_gate[..., None] - jnp.transpose(gate_block, (1, 2, 0))[None]
            key_pos = offset + jnp.arange(block_len, dtype=jnp.int32)
            allowed = key_pos[None, :] <= query_pos[:, None]
            scores = jnp.where(allowed[:, None, None, :], scores, SCORE_FLOOR)
            new_max = jnp.maximum(maxima, jnp.max(scores, axis=-1))
            factor = jnp.exp(maxima - new_max)
            weights = jnp.exp(scores - new_max[..., None])
            totals = factor * totals + jnp.sum(weights, axis=-1)
            weighted = factor[..., None] * weighted + jnp.einsum(
                "qgrk,kgd->qgrd",
                weights.astype(jnp.bfloat16),
                value_block,
                preferred_element_type=jnp.float32,
            )
            return (new_max, totals, weighted)

        return lax.cond(offset <= last_row, accumulate, lambda kept_state: kept_state, state)

    maxima, totals, weighted = lax.fori_loop(0, length // block_len, advance, initial)
    heads_out = (
        (weighted / totals[..., None])
        .astype(jnp.bfloat16)
        .reshape(local_rows, groups * group_ratio * HD)
    )
    return lax.psum_scatter(
        jnp.dot(heads_out, out_proj, preferred_element_type=jnp.float32).astype(jnp.bfloat16),
        "tp",
        scatter_dimension=0,
        tiled=True,
    )


def experts_part(tokens, norm_gain, routes, route_weights, w_gate, w_up, w_down):
    row_count = tokens.shape[0]
    feature_count = tokens.shape[1]
    top_count = routes.shape[1]
    experts = w_gate.shape[0] * lax.axis_size("ep")
    tp_count = lax.axis_size("tp")
    capacity = 2 * row_count * top_count // experts
    tokens_wide = tokens.astype(jnp.float32)
    normed = (
        tokens_wide
        * lax.rsqrt(jnp.mean(tokens_wide * tokens_wide, axis=-1, keepdims=True) + 1e-06)
        * norm_gain
    ).astype(jnp.bfloat16)
    flat_ids = routes.reshape(-1)
    onehot = (flat_ids[:, None] == jnp.arange(experts, dtype=jnp.int32)[None, :]).astype(jnp.int32)
    slot_rank = jnp.sum((jnp.cumsum(onehot, axis=0) - 1) * onehot, axis=1)
    slot_ids = flat_ids * capacity + slot_rank
    owner_row = jnp.arange(row_count * top_count, dtype=jnp.int32) // top_count
    slot_rows = jnp.full((experts * capacity,), -1, jnp.int32).at[slot_ids].set(owner_row)
    filled = slot_rows >= 0
    outgoing = jnp.where(
        filled[:, None], normed[jnp.maximum(slot_rows, 0)], jnp.zeros((), jnp.bfloat16)
    )
    share_size = capacity // tp_count
    blocks = outgoing.reshape(experts, capacity, feature_count)
    own_part = lax.dynamic_slice_in_dim(blocks, lax.axis_index("tp") * share_size, share_size, 1)
    partial_in = lax.all_to_all(own_part, "ep", split_axis=0, concat_axis=0, tiled=True)
    arrived = lax.all_gather(partial_in, "tp", axis=1, tiled=True).reshape(-1, feature_count)
    gate_act = jnp.dot(arrived, w_gate[0], preferred_element_type=jnp.float32)
    up_act = jnp.dot(arrived, w_up[0], preferred_element_type=jnp.float32)
    latent_width = (jax.nn.silu(gate_act) * up_act).astype(jnp.bfloat16)
    partial_value = jnp.dot(latent_width, w_down[0], preferred_element_type=jnp.float32)
    results = lax.psum_scatter(
        partial_value.astype(jnp.bfloat16), "tp", scatter_dimension=1, tiled=True
    )
    returned_rows = lax.all_to_all(results, "ep", split_axis=0, concat_axis=0, tiled=True)
    picked = returned_rows[slot_ids].astype(jnp.float32).reshape(row_count, top_count, -1)
    return jnp.sum(picked * route_weights[:, :, None], axis=1).astype(jnp.bfloat16)


def normalize(tokens, norm_gain):
    tokens_wide = tokens.astype(jnp.float32)
    return (
        tokens_wide
        * lax.rsqrt(jnp.mean(tokens_wide * tokens_wide, axis=-1, keepdims=True) + 1e-06)
        * norm_gain
    ).astype(jnp.bfloat16)


def combine_table(routes, route_weights, experts):
    chosen = routes[:, :, None] == jnp.arange(experts, dtype=jnp.int32)[None, None, :]
    return jnp.sum(jnp.where(chosen, route_weights[:, :, None], 0.0), axis=1)


def exchange_down(w_down):
    count = lax.axis_size("tp")
    me = lax.axis_index("tp")
    hidden, features = w_down.shape
    width = features // count
    result = jnp.zeros((count * hidden, width), w_down.dtype)
    for offset in range(count):
        target = (me + offset) % count
        block = lax.dynamic_slice_in_dim(w_down, target * width, width, 1)
        if offset:
            block = lax.ppermute(block, "tp", [(i, (i + offset) % count) for i in range(count)])
        source = (me - offset) % count
        result = lax.dynamic_update_slice_in_dim(result, block, source * hidden, 0)
    return result


def experts_dense(rows, table, w_gate, w_up, down):
    gate_act = jnp.dot(rows, w_gate[0], preferred_element_type=jnp.float32)
    up_act = jnp.dot(rows, w_up[0], preferred_element_type=jnp.float32)
    hidden = (jax.nn.silu(gate_act) * up_act).astype(jnp.bfloat16)
    full = lax.all_gather(hidden, "tp", axis=1, tiled=True)
    expert_out = jnp.dot(full, down, preferred_element_type=jnp.float32)
    mine = lax.dynamic_index_in_dim(table, lax.axis_index("ep"), 1, keepdims=True)
    return lax.psum_scatter(
        (expert_out * mine).astype(jnp.bfloat16), "ep", scatter_dimension=0, tiled=True
    )


def per_device(
    queries,
    keys,
    values,
    cum_gates,
    out_proj,
    tokens,
    norm_gain,
    routes,
    route_weights,
    w_gate,
    w_up,
    w_down,
):
    experts = w_gate.shape[0] * lax.axis_size("ep")
    row_count, top_count = routes.shape
    dense = 2 * row_count * top_count // experts >= row_count
    packed = [keys, values, split_three(cum_gates)]
    if dense:
        packed.append(split_three(combine_table(routes, route_weights, experts)))
    gathered = gather_packed(packed, "ep")
    key_rows = gathered[0].reshape(-1, keys.shape[1])
    value_rows = gathered[1].reshape(-1, values.shape[1])
    key_gates = join_three(gathered[2], 1).reshape(-1, cum_gates.shape[1])
    mixed = attend(queries, key_rows, value_rows, key_gates, cum_gates, out_proj)
    if dense:
        table = join_three(gathered[3], 1).reshape(-1, experts)
        share = row_count // lax.axis_size("tp")
        own = lax.dynamic_slice_in_dim(tokens, lax.axis_index("tp") * share, share, 0)
        rows = lax.all_gather(normalize(own, norm_gain), ("ep", "tp"), axis=0, tiled=True)
        routed = experts_dense(rows, table, w_gate, w_up, exchange_down(w_down[0]))
    else:
        routed = experts_part(
            tokens, norm_gain, routes, route_weights, w_gate, w_up, w_down
        )
    return (mixed, routed)


def solution(mesh):
    placed = (
        P("ep", "tp"),
        P("ep", "tp"),
        P("ep", "tp"),
        P("ep", "tp"),
        P("tp", None),
        P("ep", None),
        P(),
        P("ep", None),
        P("ep", None),
        P("ep", None, "tp"),
        P("ep", None, "tp"),
        P("ep", "tp", None),
    )
    return jax.shard_map(
        per_device,
        mesh=mesh,
        in_specs=placed,
        out_specs=(P(("ep", "tp"), None), P("ep", "tp")),
        check_vma=False,
    )
```

```python
import functools
import math

import jax
import jax.numpy as jnp
from jax import lax
from jax.experimental import pallas as pl
from jax.experimental.pallas import tpu as pltpu
from jax.sharding import PartitionSpec as P

HD = 128


SCORE_FLOOR = -1e30


def split_three(x):
    high = lax.reduce_precision(x, 8, 7)
    rest = x - high
    middle = lax.reduce_precision(rest, 8, 7)
    low = rest - middle
    return jnp.stack([high, middle, low]).astype(jnp.bfloat16)


def join_three(pieces, axis):
    wide = pieces.astype(jnp.float32)
    parts = [lax.index_in_dim(wide, i, axis, keepdims=False) for i in range(3)]
    return (parts[2] + parts[1]) + parts[0]


def gather_packed(arrays, axis, beside):
    lanes = 128
    rows = []
    for array in arrays:
        flat = array.reshape(-1)
        flat = jnp.pad(flat, (0, -flat.shape[0] % (16 * lanes)))
        rows.append(flat.reshape(-1, lanes))
    packed, beside = lax.optimization_barrier((jnp.concatenate(rows, axis=0), beside))
    gathered = lax.all_gather(packed, axis, axis=0, tiled=False)
    count = gathered.shape[0]
    results = []
    first = 0
    for array, block in zip(arrays, rows):
        piece = gathered[:, first : first + block.shape[0]]
        if array.size != block.size:
            piece = piece.reshape(count, -1)[:, : array.size]
        results.append(piece.reshape((count,) + array.shape))
        first += block.shape[0]
    return results, beside


def attend(queries, key_rows, value_rows, key_gates, cum_gates, out_proj, beside):
    local_rows = queries.shape[0]
    groups = key_rows.shape[1] // HD
    group_ratio = cum_gates.shape[1] // groups
    score_scale = HD ** (-0.5)
    first_row = lax.axis_index("ep") * local_rows
    last_row = first_row + local_rows - 1
    query_four = queries.reshape(local_rows, groups, group_ratio, HD)
    query_gate = cum_gates.reshape(local_rows, groups, group_ratio)
    query_pos = first_row + jnp.arange(local_rows, dtype=jnp.int32)
    initial = (
        jnp.full((local_rows, groups, group_ratio), SCORE_FLOOR, jnp.float32),
        jnp.zeros((local_rows, groups, group_ratio), jnp.float32),
        jnp.zeros((local_rows, groups, group_ratio, HD), jnp.float32),
    )
    length = key_rows.shape[0]
    block_len = math.gcd(length, 512)

    def advance(block_index, state):
        offset = block_index * block_len

        def accumulate(current):
            maxima, totals, weighted = current
            key_block = lax.dynamic_slice_in_dim(key_rows, offset, block_len, 0).reshape(
                block_len, groups, HD
            )
            value_block = lax.dynamic_slice_in_dim(value_rows, offset, block_len, 0).reshape(
                block_len, groups, HD
            )
            gate_block = lax.dynamic_slice_in_dim(key_gates, offset, block_len, 0).reshape(
                block_len, groups, group_ratio
            )
            scores = (
                jnp.einsum(
                    "qgrd,kgd->qgrk", query_four, key_block, preferred_element_type=jnp.float32
                )
                * score_scale
            )
            scores = scores + query_gate[..., None] - jnp.transpose(gate_block, (1, 2, 0))[None]
            key_pos = offset + jnp.arange(block_len, dtype=jnp.int32)
            allowed = key_pos[None, :] <= query_pos[:, None]
            scores = jnp.where(allowed[:, None, None, :], scores, SCORE_FLOOR)
            new_max = jnp.maximum(maxima, jnp.max(scores, axis=-1))
            factor = jnp.exp(maxima - new_max)
            weights = jnp.exp(scores - new_max[..., None])
            totals = factor * totals + jnp.sum(weights, axis=-1)
            weighted = factor[..., None] * weighted + jnp.einsum(
                "qgrk,kgd->qgrd",
                weights.astype(jnp.bfloat16),
                value_block,
                preferred_element_type=jnp.float32,
            )
            return (new_max, totals, weighted)

        return lax.cond(offset <= last_row, accumulate, lambda kept_state: kept_state, state)

    maxima, totals, weighted = lax.fori_loop(0, length // block_len, advance, initial)
    heads_out = (
        (weighted / totals[..., None])
        .astype(jnp.bfloat16)
        .reshape(local_rows, groups * group_ratio * HD)
    )
    heads_out, beside = lax.optimization_barrier((heads_out, beside))
    mixed = lax.psum_scatter(
        jnp.dot(heads_out, out_proj, preferred_element_type=jnp.float32).astype(jnp.bfloat16),
        "tp",
        scatter_dimension=0,
        tiled=True,
    )
    return mixed, beside


def experts_part(tokens, norm_gain, routes, route_weights, w_gate, w_up, w_down):
    row_count = tokens.shape[0]
    feature_count = tokens.shape[1]
    top_count = routes.shape[1]
    experts = w_gate.shape[0] * lax.axis_size("ep")
    tp_count = lax.axis_size("tp")
    capacity = 2 * row_count * top_count // experts
    tokens_wide = tokens.astype(jnp.float32)
    normed = (
        tokens_wide
        * lax.rsqrt(jnp.mean(tokens_wide * tokens_wide, axis=-1, keepdims=True) + 1e-06)
        * norm_gain
    ).astype(jnp.bfloat16)
    flat_ids = routes.reshape(-1)
    onehot = (flat_ids[:, None] == jnp.arange(experts, dtype=jnp.int32)[None, :]).astype(jnp.int32)
    slot_rank = jnp.sum((jnp.cumsum(onehot, axis=0) - 1) * onehot, axis=1)
    slot_ids = flat_ids * capacity + slot_rank
    owner_row = jnp.arange(row_count * top_count, dtype=jnp.int32) // top_count
    slot_rows = jnp.full((experts * capacity,), -1, jnp.int32).at[slot_ids].set(owner_row)
    filled = slot_rows >= 0
    outgoing = jnp.where(
        filled[:, None], normed[jnp.maximum(slot_rows, 0)], jnp.zeros((), jnp.bfloat16)
    )
    share_size = capacity // tp_count
    blocks = outgoing.reshape(experts, capacity, feature_count)
    own_part = lax.dynamic_slice_in_dim(blocks, lax.axis_index("tp") * share_size, share_size, 1)
    partial_in = lax.all_to_all(own_part, "ep", split_axis=0, concat_axis=0, tiled=True)
    arrived = lax.all_gather(partial_in, "tp", axis=1, tiled=True).reshape(-1, feature_count)
    gate_act = jnp.dot(arrived, w_gate[0], preferred_element_type=jnp.float32)
    up_act = jnp.dot(arrived, w_up[0], preferred_element_type=jnp.float32)
    latent_width = (jax.nn.silu(gate_act) * up_act).astype(jnp.bfloat16)
    partial_value = jnp.dot(latent_width, w_down[0], preferred_element_type=jnp.float32)
    results = lax.psum_scatter(
        partial_value.astype(jnp.bfloat16), "tp", scatter_dimension=1, tiled=True
    )
    returned_rows = lax.all_to_all(results, "ep", split_axis=0, concat_axis=0, tiled=True)
    picked = returned_rows[slot_ids].astype(jnp.float32).reshape(row_count, top_count, -1)
    return jnp.sum(picked * route_weights[:, :, None], axis=1).astype(jnp.bfloat16)


def normalize(tokens, norm_gain):
    tokens_wide = tokens.astype(jnp.float32)
    return (
        tokens_wide
        * lax.rsqrt(jnp.mean(tokens_wide * tokens_wide, axis=-1, keepdims=True) + 1e-06)
        * norm_gain
    ).astype(jnp.bfloat16)


def combine_table(routes, route_weights, experts):
    chosen = routes[:, :, None] == jnp.arange(experts, dtype=jnp.int32)[None, None, :]
    return jnp.sum(jnp.where(chosen, route_weights[:, :, None], 0.0), axis=1)


def exchange_down(w_down):
    count = lax.axis_size("tp")
    me = lax.axis_index("tp")
    hidden, features = w_down.shape
    width = features // count
    result = jnp.zeros((count * hidden, width), w_down.dtype)
    for offset in range(count):
        target = (me + offset) % count
        block = lax.dynamic_slice_in_dim(w_down, target * width, width, 1)
        if offset:
            block = lax.ppermute(block, "tp", [(i, (i + offset) % count) for i in range(count)])
        source = (me - offset) % count
        result = lax.dynamic_update_slice_in_dim(result, block, source * hidden, 0)
    return result


MESH = pl.DeviceIdType.MESH


def spread_kernel(n_ep, n_tp, share, local_ref, out_ref, send_sem, recv_sem, own_sem):
    ep = lax.axis_index("ep")
    tp = lax.axis_index("tp")
    near = tp + 1 - 2 * lax.rem(tp, 2)
    far = lax.rem(tp + 2, n_tp)
    block = share * n_tp

    barrier = pltpu.get_barrier_semaphore()
    for offset in range(1, n_ep):
        peer = lax.rem(ep + offset, n_ep)
        pl.semaphore_signal(barrier, inc=1, device_id=(peer, tp), device_id_type=MESH)
    for peer in (near, far):
        pl.semaphore_signal(barrier, inc=1, device_id=(ep, peer), device_id_type=MESH)
    pl.semaphore_wait(barrier, n_ep + 1)

    def rows(source, part):
        return pl.ds(pl.multiple_of(source * block + part * share, share), share)

    def remote(kind, offset, src, place, device):
        return pltpu.make_async_remote_copy(
            src_ref=src,
            dst_ref=out_ref.at[place],
            send_sem=send_sem.at[kind, offset - 1],
            recv_sem=recv_sem.at[kind, offset - 1],
            device_id=device,
            device_id_type=MESH,
        )

    def source_of(offset):
        return lax.rem(ep + n_ep - offset, n_ep)

    def forward(kind, offset):
        source = source_of(offset)
        if kind == 3:
            place = rows(source, far)
        else:
            place = rows(source, tp)
        target = far if kind == 1 else near
        return remote(kind, offset, out_ref.at[place], place, (ep, target))

    mine = local_ref.at[pl.ds(pl.multiple_of(tp * share, share), share)]
    first = []
    for offset in range(1, n_ep):
        peer = lax.rem(ep + offset, n_ep)
        copy = remote(0, offset, mine, rows(ep, tp), (peer, tp))
        copy.start()
        first.append(copy)
    own = pltpu.make_async_copy(
        local_ref, out_ref.at[pl.ds(pl.multiple_of(ep * block, block), block)], own_sem
    )
    own.start()
    across, beside, second = [], [], []
    for offset in range(1, n_ep):
        first[offset - 1].wait_recv()
        for kind, kept in ((1, across), (2, beside)):
            copy = forward(kind, offset)
            copy.start()
            kept.append(copy)
        if offset > 1:
            across[offset - 2].wait_recv()
            copy = forward(3, offset - 1)
            copy.start()
            second.append(copy)
    across[-1].wait_recv()
    copy = forward(3, n_ep - 1)
    copy.start()
    second.append(copy)
    for copy in beside + second:
        copy.wait_recv()
    own.wait()
    for copy in first + across + beside + second:
        copy.wait_send()


def spread_rows(local):
    n_ep, n_tp = lax.axis_size("ep"), lax.axis_size("tp")
    count, features = local.shape
    share = count // n_tp
    sent = local.size * local.dtype.itemsize * (n_ep - 1)
    return pl.pallas_call(
        functools.partial(spread_kernel, n_ep, n_tp, share),
        out_shape=jax.ShapeDtypeStruct((n_ep * count, features), local.dtype),
        in_specs=[pl.BlockSpec(memory_space=pltpu.VMEM)],
        out_specs=pl.BlockSpec(memory_space=pl.ANY),
        scratch_shapes=[
            pltpu.SemaphoreType.DMA((4, n_ep - 1)),
            pltpu.SemaphoreType.DMA((4, n_ep - 1)),
            pltpu.SemaphoreType.DMA,
        ],
        compiler_params=pltpu.CompilerParams(collective_id=0, has_side_effects=True),
        cost_estimate=pl.CostEstimate(flops=0, bytes_accessed=12 * sent, transcendentals=0),
        name="spread_rows",
    )(local)


def experts_dense(rows, table, w_gate, w_up, down):
    gate_act = jnp.dot(rows, w_gate[0], preferred_element_type=jnp.float32)
    up_act = jnp.dot(rows, w_up[0], preferred_element_type=jnp.float32)
    hidden = (jax.nn.silu(gate_act) * up_act).astype(jnp.bfloat16)
    full = lax.all_gather(hidden, "tp", axis=1, tiled=True)
    expert_out = jnp.dot(full, down, preferred_element_type=jnp.float32)
    mine = lax.dynamic_index_in_dim(table, lax.axis_index("ep"), 1, keepdims=True)
    returned = lax.all_to_all(
        (expert_out * mine).astype(jnp.bfloat16), "ep", split_axis=0, concat_axis=0, tiled=True
    )
    terms = returned.reshape(lax.axis_size("ep"), -1, returned.shape[1]).astype(jnp.float32)
    return jnp.sum(terms, axis=0).astype(jnp.bfloat16)


def per_device(
    queries,
    keys,
    values,
    cum_gates,
    out_proj,
    tokens,
    norm_gain,
    routes,
    route_weights,
    w_gate,
    w_up,
    w_down,
):
    experts = w_gate.shape[0] * lax.axis_size("ep")
    row_count, top_count = routes.shape
    dense = 2 * row_count * top_count // experts >= row_count
    packed = [keys, values, split_three(cum_gates)]
    if dense:
        packed.append(split_three(combine_table(routes, route_weights, experts)))
    tp_count = lax.axis_size("tp")
    own = normalize(tokens, norm_gain) if dense else tokens
    gathered, own = gather_packed(packed, "ep", own)
    key_rows = gathered[0].reshape(-1, keys.shape[1])
    value_rows = gathered[1].reshape(-1, values.shape[1])
    key_gates = join_three(gathered[2], 1).reshape(-1, cum_gates.shape[1])
    if dense:
        table = join_three(gathered[3], 1).reshape(-1, experts)
        if tp_count == 4 and row_count % (16 * tp_count) == 0:
            rows = spread_rows(own)
        else:
            rows = lax.all_gather(own, "ep", axis=0, tiled=True)
        rows, down_shard = lax.optimization_barrier((rows, w_down[0]))
        down = exchange_down(down_shard)
        mixed, down = attend(
            queries, key_rows, value_rows, key_gates, cum_gates, out_proj, down
        )
        routed = experts_dense(rows, table, w_gate, w_up, down)
    else:
        mixed, _ = attend(
            queries, key_rows, value_rows, key_gates, cum_gates, out_proj, w_down
        )
        routed = experts_part(
            tokens, norm_gain, routes, route_weights, w_gate, w_up, w_down
        )
    return (mixed, routed)


def solution(mesh):
    placed = (
        P("ep", "tp"),
        P("ep", "tp"),
        P("ep", "tp"),
        P("ep", "tp"),
        P("tp", None),
        P("ep", None),
        P(),
        P("ep", None),
        P("ep", None),
        P("ep", None, "tp"),
        P("ep", None, "tp"),
        P("ep", "tp", None),
    )
    return jax.shard_map(
        per_device,
        mesh=mesh,
        in_specs=placed,
        out_specs=(P(("ep", "tp"), None), P("ep", "tp")),
        check_vma=False,
    )
```
